32 devices in a mesh: sp: 4 (over y, core), dp: 8 (over z, x).
Axes of the slice: x: 2, y: 2, z: 4, core: 2. Of those that a mesh axis runs over, the one named last changes fastest.
Arguments:
- standardized_block_source: bfloat16 [16, 256, 2064], P('dp', 'sp'), may hold values from -6 to 6
- forgetting_narrowing_matrix: bfloat16 [2064, 32], P('dp'), may hold values from -0.125 to 0.125
- forgetting_widening_matrix: bfloat16 [32, 1024], replicated, may hold values from -1 to 1
- forgetting_offset_vector: float32 [1024], replicated, may hold values from -1.5 to 6.5
- probe_vectors: bfloat16 [128, 256, 128], P(('dp', 'sp')), may hold values from -6 to 6
- address_vectors: bfloat16 [128, 256, 128], P(('dp', 'sp')), may hold values from -6 to 6
- payload_vectors: bfloat16 [128, 256, 256], P(('dp', 'sp')), may hold values from -6 to 6
- extra_channel_forgetting: float32 [128, 256], P(('dp', 'sp')), may hold values from -2.1 to 0
- blender_result_adjoint: bfloat16 [16, 256, 2048], P('dp', 'sp'), may hold values from -0.29882812 to 0.29882812
Outputs:
- grad_queries: bfloat16 [16, 256, 1024], P('dp', 'sp')
- grad_keys: bfloat16 [16, 256, 1024], P('dp', 'sp')
- grad_values: bfloat16 [16, 256, 2048], P('dp', 'sp')
- grad_input: bfloat16 [16, 256, 2064], P('dp', 'sp')
- grad_gate_down: float32 [2064, 32], P('dp')
- grad_gate_up: float32 [32, 1024], replicated
- grad_gate_bias: float32 [1024], replicated
The draws below stay inside these ranges and needn't reach their ends.
All inputs are finite; a program needn't handle non-finite values.
Results may differ from the reference program's by a relative error of at most 0.0069.
Values may be sent and summed in bfloat16 or wider, within the bound.
A program may use at most 64 MiB of HBM per device.

```python
import jax
import jax.numpy as jnp
from jax import lax

D = 2064
HEADS = 8
ADDRESS_WIDTH = 128
PAYLOAD_WIDTH = 256
RANK = 32
BLOCK = 64
LEN = 256
BATCH = 16
KD = 1024
VD = 2048


def draw_forgetting_offset_vector(key, part):
    pick_key, level_key, jitter_key = jax.random.split(jax.random.fold_in(key, 11), 3)
    slow_share = 0.5
    slow_heads = jax.random.uniform(pick_key, (HEADS,)) < slow_share
    slow_level = jax.random.uniform(level_key, (HEADS,), minval=4.5, maxval=6.0)
    fast_level = jax.random.uniform(jax.random.fold_in(level_key, 1), (HEADS,), minval=-1.0, maxval=0.5)
    levels = jnp.where(slow_heads, slow_level, fast_level)
    jitter = jax.random.uniform(jitter_key, (HEADS, ADDRESS_WIDTH), minval=-0.5, maxval=0.5)
    return (levels[:, None] + jitter).reshape(HEADS * ADDRESS_WIDTH).astype(jnp.float32)


def draw_extra_channel_forgetting(key, part):
    place_key, loss_key = jax.random.split(jax.random.fold_in(key, 23))
    item_rows = BATCH * HEADS
    positions = jax.random.randint(place_key, (item_rows, 3, 1), 0, LEN)
    losses = jnp.log(jax.random.uniform(loss_key, (item_rows, 3, 1), minval=0.5, maxval=0.8))
    places = jnp.arange(LEN, dtype=jnp.int32)[None, None, :]
    return jnp.sum(jnp.where(places == positions, losses, 0.0), axis=1).astype(jnp.float32)


def strengthened(values, own_key, source, target, shards_of, factor):
    def block_of(position):
        return (jnp.arange(values.shape[position]) // (values.shape[position] // shards_of)).reshape((-1,) + (1,) * (values.ndim - 1 - position))

    first = jax.random.permutation(own_key, shards_of)[block_of(target)]
    second = (block_of(target) + shards_of // 2) % shards_of
    return jnp.where((block_of(source) == first) | (block_of(source) == second), factor * values, values)


def block_levels(key, shape, cuts, low, high):
    def one(position, parts):
        draws = jax.random.uniform(jax.random.fold_in(jax.random.fold_in(key, 6), position), (parts,), jnp.float32, low / len(cuts), high / len(cuts))
        return jnp.repeat(jnp.exp(draws), shape[position] // parts).reshape((-1,) + (1,) * (len(shape) - position - 1))

    loudness = one(*cuts[0])
    for cut in cuts[1:]:
        loudness = loudness * one(*cut)
    return loudness


def gaussian(own_key, extent, width, reach, cuts=(), kind=jnp.bfloat16):
    loudness = block_levels(own_key, extent, cuts, -0.22, 0.18) if cuts else 1.0
    result = jax.random.normal(own_key, extent, jnp.float32) * width * loudness
    return jnp.minimum(jnp.maximum(result, -reach), reach).astype(kind)


def heavy_noise(own_key, shape, width, most, cuts, heavy, kind=jnp.bfloat16):
    values = width * jax.random.normal(own_key, shape, jnp.float32)
    if cuts:
        values = values * block_levels(own_key, shape, cuts, -0.22, 0.18)
    return jnp.clip(strengthened(values, jax.random.fold_in(own_key, 3), *heavy), -most, most).astype(kind)


def setup_inputs(seed: int = 0) -> dict:
    keys = jax.random.split(jax.random.key(seed), 10)
    return {
        "standardized_block_source": heavy_noise(keys[0], (BATCH, LEN, D), 1.0, 6.0, ((0, 8), (1, 4)), (0, 2, 8, 2.0)),
        "forgetting_narrowing_matrix": gaussian(keys[1], (D, RANK), D ** -0.5, 0.125, ((0, 8),)),
        "forgetting_widening_matrix": gaussian(keys[2], (RANK, KD), RANK ** -0.5, 1.0),
        "forgetting_offset_vector": draw_forgetting_offset_vector(jax.random.fold_in(keys[9], 71), 0),
        "probe_vectors": gaussian(keys[4], (BATCH * HEADS, LEN, ADDRESS_WIDTH), 1.0, 6.0, ((0, 32),)),
        "address_vectors": gaussian(keys[5], (BATCH * HEADS, LEN, ADDRESS_WIDTH), 1.0, 6.0, ((0, 32),)),
        "payload_vectors": gaussian(keys[6], (BATCH * HEADS, LEN, PAYLOAD_WIDTH), 1.0, 6.0, ((0, 32),)),
        "extra_channel_forgetting": draw_extra_channel_forgetting(jax.random.fold_in(keys[9], 71), 0),
        "blender_result_adjoint": gaussian(keys[8], (BATCH, LEN, VD), 0.05, 0.29882812, ((0, 8), (1, 4))),
    }


retention_smoothing = 16.0

def head_forward(stream_probe_entries, stream_address_entries, stream_payload_entries, retention_coefficient):
    length, key_width = stream_probe_entries.shape
    value_width = stream_payload_entries.shape[1]
    blocks = length // BLOCK
    scaled = stream_probe_entries * key_width ** (-0.5)
    causal = jnp.tril(jnp.ones((BLOCK, BLOCK), dtype=bool))
    highest = lax.Precision.HIGHEST

    def advance(memory, pieces):
        query_block, key_block, value_block, decay_sums = pieces
        spread = decay_sums[:, None, :] - decay_sums[None, :, :]
        decays = jnp.exp(jnp.where(causal[:, :, None], spread, -jnp.inf))
        scores = jnp.einsum('td,sd,tsd->ts', query_block, key_block, decays, precision=highest)
        within = jnp.dot(scores, value_block, precision=highest)
        carried = jnp.dot(query_block * jnp.exp(decay_sums), memory, precision=highest)
        ending = decay_sums[-1]
        fading = key_block * jnp.exp(ending[None, :] - decay_sums)
        memory = memory * jnp.exp(ending)[:, None] + jnp.dot(fading.T, value_block, precision=highest)
        return (memory, within + carried)

    def blocked(tensor):
        return tensor.reshape(blocks, BLOCK, tensor.shape[1])
    initial = jnp.zeros((key_width, value_width), jnp.float32)
    decay_sums = jnp.cumsum(blocked(retention_coefficient), axis=1)
    _, outputs = lax.scan(jax.checkpoint(advance), initial, (blocked(scaled), blocked(stream_address_entries), blocked(stream_payload_entries), decay_sums))
    return outputs.reshape(length, value_width)

def stream_sensitivities(stream_probe_entries, stream_address_entries, stream_payload_entries, forgetting_logit_values, surplus_retention_loss, result_adjoint):

    def forward(query_in, key_in, value_in, retention_basis_components):
        retention_coefficient = jax.nn.log_sigmoid(retention_basis_components) / retention_smoothing + surplus_retention_loss[:, None]
        return head_forward(query_in, key_in, value_in, retention_coefficient)
    _, pullback = jax.vjp(forward, stream_probe_entries.astype(jnp.float32), stream_address_entries.astype(jnp.float32), stream_payload_entries.astype(jnp.float32), forgetting_logit_values)
    query_grad, key_grad, value_grad, gate_grad = pullback(result_adjoint.astype(jnp.float32))
    return (query_grad.astype(jnp.bfloat16), key_grad.astype(jnp.bfloat16), value_grad.astype(jnp.bfloat16), gate_grad.astype(jnp.bfloat16))

def reference(standardized_block_source, forgetting_narrowing_matrix, forgetting_widening_matrix, forgetting_offset_vector, probe_vectors, address_vectors, payload_vectors, extra_channel_forgetting, blender_result_adjoint):
    batch, length, model_width = standardized_block_source.shape
    flat_input = standardized_block_source.reshape(batch * length, model_width)
    low_rank = jnp.dot(flat_input, forgetting_narrowing_matrix, preferred_element_type=jnp.float32).astype(jnp.bfloat16)
    logit_by_position = jnp.dot(low_rank, forgetting_widening_matrix, preferred_element_type=jnp.float32) + forgetting_offset_vector

    def regroup_into_entries(tensor, columns):
        return tensor.reshape(batch, length, HEADS, columns).transpose(0, 2, 1, 3).reshape(batch * HEADS, length, columns)

    def to_tokens(tensor):
        columns = tensor.shape[2]
        return tensor.reshape(batch, HEADS, length, columns).transpose(0, 2, 1, 3).reshape(batch, length, HEADS * columns)

    def single_sample_entries(pieces):
        return stream_sensitivities(pieces[0], pieces[1], pieces[2], pieces[3], pieces[4], pieces[5])
    weight_sensitivities = lax.map(single_sample_entries, (probe_vectors, address_vectors, payload_vectors, regroup_into_entries(logit_by_position, ADDRESS_WIDTH), extra_channel_forgetting, regroup_into_entries(blender_result_adjoint, PAYLOAD_WIDTH)))
    gate_tokens = to_tokens(weight_sensitivities[3]).reshape(batch * length, HEADS * ADDRESS_WIDTH)
    low_grad = jnp.dot(gate_tokens, forgetting_widening_matrix.T, preferred_element_type=jnp.float32).astype(jnp.bfloat16)
    incoming_sensitivity = jnp.dot(low_grad, forgetting_narrowing_matrix.T, preferred_element_type=jnp.float32).astype(jnp.bfloat16)
    contract = (((0,), (0,)), ((), ()))
    down_grad = lax.dot_general(flat_input, low_grad, contract, preferred_element_type=jnp.float32)
    up_grad = lax.dot_general(low_rank, gate_tokens, contract, preferred_element_type=jnp.float32)
    bias_grad = lax.optimization_barrier(jnp.sum(gate_tokens.astype(jnp.float32), axis=0))
    return (to_tokens(weight_sensitivities[0]), to_tokens(weight_sensitivities[1]), to_tokens(weight_sensitivities[2]), incoming_sensitivity.reshape(batch, length, model_width), down_grad, up_grad, bias_grad)
```

```python
import functools

import jax
import jax.numpy as jnp
from jax import lax
from jax.experimental import pallas as pl
from jax.experimental.pallas import tpu as pltpu
from jax.sharding import PartitionSpec as P

HEADS = 8
KW = 128
VW = 256
BLOCK = 64
SMOOTH = 16.0
MESH = pl.DeviceIdType.MESH
F32 = jnp.float32
BF = jnp.bfloat16
NN = (((1,), (0,)), ((), ()))
NT = (((1,), (1,)), ((), ()))
TN = (((0,), (0,)), ((), ()))


def dot(a, b, dims=NN):
    return lax.dot_general(a, b, dims, preferred_element_type=F32)


def split(x, parts):
    out = []
    for _ in range(parts - 1):
        hi = x.astype(BF)
        out.append(hi)
        x = x - hi.astype(F32)
    out.append(x.astype(BF))
    return out


def kernel(
    n_sp, n_dp, seqs, rows,
    xp_ref, dt_ref, up_ref, offs_ref, q_ref, k_ref, v_ref, extra_ref, adj_ref,
    gqkv_ref, gi_ref, gd_ref, gu_ref,
    down_all, low_all, adj_in, gbuf, state, states, dstate, bsum, slope, gpre,
    glp, glp_in, gdp, gd_in, gd_sum, ub, ub_in, ub_sum,
    s_down, r_down, s_adj, r_adj, s_low, r_low, s_g, r_g, s_gl, r_gl,
    s_gd, r_gd, s_gs, r_gs, s_ub, r_ub, s_us, r_us,
):
    sp, dp = lax.axis_index("sp"), lax.axis_index("dp")
    n_all = n_sp * n_dp
    me = dp * n_sp + sp
    rank = dt_ref.shape[0]
    nj = rank // 8
    blocks = n_sp
    seq_of_me = (sp * rows) // HEADS
    head0 = lax.rem(sp * rows, HEADS)
    scale = KW ** (-0.5)

    def remote(src, dst, ss, rs, to_sp, to_dp):
        return pltpu.make_async_remote_copy(
            src_ref=src, dst_ref=dst, send_sem=ss, recv_sem=rs,
            device_id={"sp": to_sp, "dp": to_dp}, device_id_type=MESH,
        )

    barrier = pltpu.get_barrier_semaphore()

    @pl.loop(1, n_all)
    def _(d):
        other = lax.rem(me + d, n_all)
        pl.semaphore_signal(
            barrier, inc=1,
            device_id={"sp": lax.rem(other, n_sp), "dp": other // n_sp}, device_id_type=MESH,
        )

    pl.semaphore_wait(barrier, n_all - 1)

    def down_copy(d):
        to = lax.rem(dp + d, n_dp)
        return remote(dt_ref, down_all.at[dp], s_down.at[d], r_down.at[dp], sp, to)

    @pl.loop(1, n_dp)
    def _(d):
        down_copy(d).start()

    def adj_copy(d):
        to = lax.rem(sp + d, n_sp)
        return remote(
            adj_ref.at[pl.ds(to * rows, rows)], adj_in.at[sp], s_adj.at[d], r_adj.at[sp], to, dp
        )

    for d in range(1, n_sp):
        adj_copy(d).start()

    down_all[dp] = dt_ref[...]
    adj_in[sp] = adj_ref[pl.ds(sp * rows, rows)]

    tokens = seqs * BLOCK

    def wait_recv(dst, sem):
        remote(dst, dst, sem, sem, sp, dp).wait_recv()

    def low_step(d, acc):
        i = lax.rem(dp + d, n_dp)

        @pl.when(d > 0)
        def _():
            wait_recv(down_all.at[i], r_down.at[i])

        return acc + dot(xp_ref[i], down_all[i], NT)

    low = lax.fori_loop(0, n_dp, low_step, jnp.zeros((tokens, rank), F32)).astype(BF)
    low_all[sp] = low

    def low_copy(d):
        to = lax.rem(sp + d, n_sp)
        return remote(low_all.at[sp], low_all.at[sp], s_low.at[d], r_low.at[sp], to, dp)

    for d in range(1, n_sp):
        low_copy(d).start()

    r_i = lax.broadcasted_iota(jnp.int32, (BLOCK, BLOCK), 0)
    c_i = lax.broadcasted_iota(jnp.int32, (BLOCK, BLOCK), 1)
    causal = r_i >= c_i
    tril = causal.astype(F32).astype(BF)
    triu = (c_i >= r_i).astype(F32).astype(BF)
    below = (r_i > c_i).astype(F32).astype(BF)
    sum_mat = jnp.concatenate([tril] * 3, axis=1)
    grad_mat = jnp.concatenate([triu, triu, below, below], axis=1)
    up_mine = up_ref[:, pl.ds(pl.multiple_of(head0 * KW, KW), rows * KW)]
    offs_mine = offs_ref[:, pl.ds(pl.multiple_of(head0 * KW, KW), rows * KW)]
    state[...] = jnp.zeros_like(state)
    dstate[...] = jnp.zeros_like(dstate)

    @pl.loop(0, blocks)
    def _(t):
        @pl.when(t != sp)
        def _():
            wait_recv(low_all.at[t], r_low.at[t])

        low_t = low_all[t, pl.ds(pl.multiple_of(seq_of_me * BLOCK, BLOCK), BLOCK), :]
        pre = dot(low_t, up_mine) + offs_mine
        at = pl.ds(pl.multiple_of(t * BLOCK, BLOCK), BLOCK)
        e = jnp.exp(-jnp.abs(pre))
        logsig = jnp.minimum(pre, 0.0) - jnp.log1p(e)
        slope[t] = jnp.where(pre >= 0, e, 1.0) / (1.0 + e) * (1.0 / SMOOTH)
        ld = logsig * (1.0 / SMOOTH) + jnp.concatenate(
            [jnp.broadcast_to(extra_ref[i, at, :], (BLOCK, KW)) for i in range(rows)], axis=1
        )
        sums = dot(sum_mat, jnp.concatenate(split(ld, 3), axis=0))
        bsum[t] = sums
        for i in range(rows):
            b = sums[:, i * KW : (i + 1) * KW]
            last = b[BLOCK - 1 : BLOCK, :]
            kh = (k_ref[i, at, :].astype(F32) * jnp.exp(last - b)).astype(BF)
            s = state[i]
            states[t, i] = s.astype(BF)
            state[i] = s * jnp.exp(last) + dot(v_ref[i, at, :], kh, TN)

    def g_copy(t):
        return remote(
            gbuf.at[t], gqkv_ref.at[pl.ds(sp * rows, rows)], s_g.at[t], r_g.at[sp], t, dp
        )

    def gl_copy(t):
        return remote(glp.at[t], glp_in.at[sp], s_gl.at[t], r_gl.at[sp], t, dp)

    middle = BLOCK // 2

    @pl.loop(0, blocks)
    def _(step):
        t = blocks - 1 - step

        @pl.when(t != sp)
        def _():
            wait_recv(adj_in.at[t], r_adj.at[t])

        at = pl.ds(pl.multiple_of(t * BLOCK, BLOCK), BLOCK)
        gl = jnp.zeros((BLOCK, rank), F32)
        for i in range(rows):
            cols = slice(i * KW, (i + 1) * KW)
            b = bsum[t, :, cols]
            last = b[BLOCK - 1 : BLOCK, :]
            centre = b[middle : middle + 1, :]
            qs = q_ref[i, at, :].astype(F32) * scale
            kk = k_ref[i, at, :].astype(F32)
            vv = v_ref[i, at, :]
            do = adj_in[t, i]
            e_ql = jnp.exp(b - centre)
            e_kl = jnp.exp(centre - b)
            e_qh = jnp.exp(b)
            e_kh = jnp.exp(last - b)
            e_last = jnp.exp(last)
            ql = (qs * e_ql).astype(BF)
            kl = (kk * e_kl).astype(BF)
            qh = (qs * e_qh).astype(BF)
            kh = (kk * e_kh).astype(BF)
            ds = dstate[i]
            dsb = ds.astype(BF)
            st = states[t, i]
            a = jnp.where(causal, dot(ql, kl, NT), 0.0).astype(BF)
            da = jnp.where(causal, dot(do, vv, NT), 0.0).astype(BF)
            dql = dot(da, kl)
            dkl = dot(da, ql, TN)
            dqh = dot(do, st)
            dkh = dot(vv, dsb)
            gv = dot(a, do, TN) + dot(kh, dsb, NT)
            gq = (dql * e_ql + dqh * e_qh) * scale
            gk = dkl * e_kl + dkh * e_kh
            gbuf[t, i, :, 0:KW] = gq.astype(BF)
            gbuf[t, i, :, KW : 2 * KW] = gk.astype(BF)
            gbuf[t, i, :, 2 * KW : 2 * KW + VW] = gv.astype(BF)
            carried = jnp.sum(ds * st.astype(F32), axis=0, keepdims=True) * e_last
            dstate[i] = ds * e_last + dot(do, qh, TN)
            w1 = ql.astype(F32) * dql - kl.astype(F32) * dkl + qh.astype(F32) * dqh
            w2 = kh.astype(F32) * dkh
            gld = dot(grad_mat, jnp.concatenate(split(w1, 2) + split(w2, 2), axis=0)) + carried
            gp = (gld * slope[t, :, cols]).astype(BF)
            gpre[i, at, :] = gp
            gl += dot(gp, up_mine[:, cols], NT)
        glp[t] = gl

        @pl.when(t != sp)
        def _():
            gl_copy(t).start()
            g_copy(t).start()

        @pl.when(t == sp)
        def _():
            glp_in[t] = gl
            gqkv_ref[pl.ds(sp * rows, rows)] = gbuf[t]

    low_seq = low_all[:, pl.ds(pl.multiple_of(seq_of_me * BLOCK, BLOCK), BLOCK), :].reshape(
        blocks * BLOCK, rank
    )

    def ub_copy(i, j):
        return remote(
            ub.at[i, j], ub_in.at[dp * seqs + seq_of_me],
            s_ub.at[i, j], r_ub.at[dp * seqs + seq_of_me], j, head0 + i,
        )

    def ub_self(i, j):
        return jnp.logical_and(head0 + i == dp, sp == j)

    for i in range(rows):
        part = dot(low_seq, gpre[i], TN)
        bias = jnp.sum(gpre[i].astype(F32), axis=0, keepdims=True)
        for j in range(nj):
            ub[i, j, 0:8, :] = part[j * 8 : (j + 1) * 8, :]
            ub[i, j, 8:16, :] = jnp.broadcast_to(bias, (8, KW))
    for i in range(rows):
        for j in range(nj):

            @pl.when(jnp.logical_not(ub_self(i, j)))
            def _():
                ub_copy(i, j).start()

            @pl.when(ub_self(i, j))
            def _():
                ub_in[dp * seqs + seq_of_me] = ub[i, j]

    for s in range(n_sp):

        @pl.when(s != sp)
        def _():
            wait_recv(glp_in.at[s], r_gl.at[s])

    per_seq = n_sp // seqs
    glow = jnp.concatenate(
        [
            functools.reduce(
                lambda x, y: x + y, [glp_in[s] for s in range(b * per_seq, (b + 1) * per_seq)]
            )
            for b in range(seqs)
        ],
        axis=0,
    ).astype(BF)

    def gd_copy(i, j):
        return remote(
            gdp.at[i, j], gd_in.at[me], s_gd.at[i, j], r_gd.at[me], j, i
        )

    @pl.loop(0, n_dp)
    def _(d):
        i = lax.rem(dp + d, n_dp)
        gdp[i] = dot(glow, xp_ref[i], TN).reshape(nj, 8, xp_ref.shape[2])
        for j in range(nj):
            own = jnp.logical_and(i == dp, sp == j)

            @pl.when(jnp.logical_not(own))
            def _():
                gd_copy(i, j).start()

            @pl.when(own)
            def _():
                gd_in[me] = gdp[i, j]

    ub_owner = jnp.logical_and(dp < HEADS, sp < nj)

    @pl.when(ub_owner)
    def _():
        for b in range(seqs):
            holder = (b * HEADS + dp) // rows

            @pl.loop(0, n_dp)
            def _(d):
                @pl.when(jnp.logical_not(jnp.logical_and(d == dp, holder == sp)))
                def _():
                    wait_recv(ub_in.at[d * seqs + b], r_ub.at[d * seqs + b])

        ub_sum[...] = jnp.sum(ub_in[...], axis=0)
        gu_ref[dp, sp] = ub_sum[...]

        @pl.loop(1, n_all)
        def _(d):
            other = lax.rem(me + d, n_all)
            remote(
                ub_sum, gu_ref.at[dp, sp], s_us.at[d], r_us.at[dp, sp],
                lax.rem(other, n_sp), other // n_sp,
            ).start()

    @pl.loop(0, n_dp)
    def _(i):
        gi_ref[i] = dot(glow, down_all[i]).astype(BF)

    @pl.when(sp < nj)
    def _():
        @pl.loop(1, n_all)
        def _(d):
            other = lax.rem(me + d, n_all)
            wait_recv(gd_in.at[other], r_gd.at[other])

        gd_sum[...] = jnp.sum(gd_in[...], axis=0)
        gd_ref[sp] = gd_sum[...]
        for d in range(1, n_sp):
            remote(
                gd_sum, gd_ref.at[sp], s_gs.at[d], r_gs.at[sp], lax.rem(sp + d, n_sp), dp
            ).start()

    for j in range(nj):

        @pl.when(j != sp)
        def _():
            wait_recv(gd_ref.at[j], r_gs.at[j])

    @pl.loop(0, HEADS)
    def _(h):
        for j in range(nj):

            @pl.when(jnp.logical_not(jnp.logical_and(h == dp, j == sp)))
            def _():
                wait_recv(gu_ref.at[h, j], r_us.at[h, j])

    for s in range(n_sp):

        @pl.when(s != sp)
        def _():
            wait_recv(gqkv_ref.at[pl.ds(s * rows, rows)], r_g.at[s])

    def sent(src, sem):
        remote(src, src, sem, sem, sp, dp).wait_send()

    @pl.loop(1, n_dp)
    def _(d):
        sent(dt_ref, s_down.at[d])

    for d in range(1, n_sp):
        sent(adj_ref.at[pl.ds(0, rows)], s_adj.at[d])
        sent(low_all.at[sp], s_low.at[d])

    @pl.loop(0, blocks)
    def _(t):
        @pl.when(t != sp)
        def _():
            sent(gbuf.at[t], s_g.at[t])
            sent(glp.at[t], s_gl.at[t])

    for i in range(rows):
        for j in range(nj):

            @pl.when(jnp.logical_not(ub_self(i, j)))
            def _():
                sent(ub.at[i, j], s_ub.at[i, j])

    @pl.loop(0, n_dp)
    def _(i):
        for j in range(nj):

            @pl.when(jnp.logical_not(jnp.logical_and(i == dp, sp == j)))
            def _():
                sent(gdp.at[i, j], s_gd.at[i, j])

    @pl.when(ub_owner)
    def _():
        @pl.loop(1, n_all)
        def _(d):
            sent(ub_sum, s_us.at[d])

    @pl.when(sp < nj)
    def _():
        for d in range(1, n_sp):
            sent(gd_sum, s_gs.at[d])


def on_device(n_sp, n_dp, x, down, up, offs, q, k, v, extra, adj):
    seqs, local_len, width = x.shape
    rows, length, _ = q.shape
    piece, rank = down.shape
    wide = -(-piece // 128) * 128
    tokens = seqs * local_len
    nj = rank // 8
    n_all = n_sp * n_dp
    items = seqs * HEADS
    assert local_len == BLOCK and HEADS % rows == 0 and n_sp % seqs == 0
    assert n_dp >= HEADS and n_sp >= nj
    xp = jnp.pad(
        x.reshape(tokens, n_dp, piece).transpose(1, 0, 2), ((0, 0), (0, 0), (0, wide - piece))
    )
    dt = jnp.pad(down.T, ((0, 0), (0, wide - piece)))
    adj_items = (
        adj.reshape(seqs, local_len, HEADS, VW).transpose(0, 2, 1, 3).reshape(items, local_len, VW)
    )
    cat = 2 * KW + VW
    vm = pl.BlockSpec(memory_space=pltpu.VMEM)
    dma = pltpu.SemaphoreType.DMA
    gqkv, gi, gd, gu = pl.pallas_call(
        functools.partial(kernel, n_sp, n_dp, seqs, rows),
        out_shape=(
            jax.ShapeDtypeStruct((items, BLOCK, cat), BF),
            jax.ShapeDtypeStruct((n_dp, tokens, wide), BF),
            jax.ShapeDtypeStruct((nj, 8, wide), F32),
            jax.ShapeDtypeStruct((HEADS, nj, 16, KW), F32),
        ),
        in_specs=[vm] * 9,
        out_specs=(vm,) * 4,
        scratch_shapes=[
            pltpu.VMEM((n_dp, rank, wide), BF),
            pltpu.VMEM((n_sp, tokens, rank), BF),
            pltpu.VMEM((n_sp, rows, BLOCK, VW), BF),
            pltpu.VMEM((n_sp, rows, BLOCK, cat), BF),
            pltpu.VMEM((rows, VW, KW), F32),
            pltpu.VMEM((n_sp, rows, VW, KW), BF),
            pltpu.VMEM((rows, VW, KW), F32),
            pltpu.VMEM((n_sp, BLOCK, rows * KW), F32),
            pltpu.VMEM((n_sp, BLOCK, rows * KW), F32),
            pltpu.VMEM((rows, length, KW), BF),
            pltpu.VMEM((n_sp, BLOCK, rank), F32),
            pltpu.VMEM((n_sp, BLOCK, rank), F32),
            pltpu.VMEM((n_dp, nj, 8, wide), F32),
            pltpu.VMEM((n_all, 8, wide), F32),
            pltpu.VMEM((8, wide), F32),
            pltpu.VMEM((rows, nj, 16, KW), F32),
            pltpu.VMEM((n_dp * seqs, 16, KW), F32),
            pltpu.VMEM((16, KW), F32),
            dma((n_dp,)), dma((n_dp,)),
            dma((n_sp,)), dma((n_sp,)),
            dma((n_sp,)), dma((n_sp,)),
            dma((n_sp,)), dma((n_sp,)),
            dma((n_sp,)), dma((n_sp,)),
            dma((n_dp, nj)), dma((n_all,)),
            dma((n_sp,)), dma((nj,)),
            dma((rows, nj)), dma((n_dp * seqs,)),
            dma((n_all,)), dma((HEADS, nj)),
        ],
        compiler_params=pltpu.CompilerParams(
            collective_id=0, has_side_effects=True, vmem_limit_bytes=56 * 1024 * 1024
        ),
    )(xp, dt, up, offs.reshape(1, -1), q, k, v, extra.reshape(rows, length, 1), adj_items)

    g = gqkv.reshape(seqs, HEADS, local_len, cat).transpose(0, 2, 1, 3)
    gi = gi[:, :, :piece].transpose(1, 0, 2).reshape(seqs, local_len, width)
    gd = gd.reshape(rank, wide)[:, :piece].T
    up_grad = gu[:, :, :8].transpose(1, 2, 0, 3).reshape(rank, HEADS * KW)
    bias = gu[:, 0, 8].reshape(HEADS * KW)
    return (
        g[..., :KW].reshape(seqs, local_len, HEADS * KW),
        g[..., KW : 2 * KW].reshape(seqs, local_len, HEADS * KW),
        g[..., 2 * KW :].reshape(seqs, local_len, HEADS * VW),
        gi,
        gd,
        up_grad,
        bias,
    )


def solution(mesh):
    tok = P("dp", "sp", None)
    item = P(("dp", "sp"), None, None)
    return jax.shard_map(
        functools.partial(on_device, mesh.shape["sp"], mesh.shape["dp"]),
        mesh=mesh,
        in_specs=(tok, P("dp", None), P(), P(), item, item, item, P(("dp", "sp"), None), tok),
        out_specs=(tok, tok, tok, tok, P("dp", None), P(), P()),
        check_vma=False,
    )
```
